1024 devices in a mesh: tp: 32 (over z, core), dp: 32 (over y, x).
Axes of the slice: x: 4, y: 8, z: 16, core: 2. Of those that a mesh axis runs over, the one named last changes fastest.
Arguments:
- tokens: bfloat16 [256, 4096], P('tp', 'dp'), may hold values from -30 to 30
- lengths: int32 [256], P('dp'), may hold values from 1 to 8192, 524288 in all
- in_gain: float32 [2, 4096], P(None, 'dp'), may hold values from 0.1 to 1.9
- w_recept: bfloat16 [2, 4096, 2048], P(None, 'dp', 'tp'), may hold values from -0.09375 to 0.09375
- w_key: bfloat16 [2, 4096, 2048], P(None, 'dp', 'tp'), may hold values from -0.09375 to 0.09375
- w_value: bfloat16 [2, 4096, 2048], P(None, 'dp', 'tp'), may hold values from -0.09375 to 0.09375
- w_decay: bfloat16 [2, 4096, 2048], P(None, 'dp', 'tp'), may hold values from -0.09375 to 0.09375
- w_rate: bfloat16 [2, 4096, 2048], P(None, 'dp', 'tp'), may hold values from -0.09375 to 0.09375
- w_gate: bfloat16 [2, 4096, 2048], P(None, 'dp', 'tp'), may hold values from -0.09375 to 0.09375
- w_out: bfloat16 [2, 2048, 4096], P(None, 'tp', 'dp'), may hold values from -0.125 to 0.125
- decay_base: float32 [2, 2048], P(None, 'tp'), may hold values from -6 to 6
- mix_gain: float32 [2, 2048], P(None, 'tp'), may hold values from 0.1 to 1.9
- states: float32 [2, 256, 32, 64, 64], P(None, 'dp', 'tp'), may hold values from -6 to 6
Outputs:
- next_tokens: bfloat16 [256, 4096], P('tp', 'dp')
- new_states: float32 [2, 256, 32, 64, 64], P(None, 'dp', 'tp')
The draws below stay inside these ranges and needn't reach their ends.
All inputs are finite; a program needn't handle non-finite values. No bound on the sum of `lengths` on one device may be relied on, other than what follows from the above.
Results may differ from the reference program's by a relative error of at most 0.0065.
Values may be sent and summed in bfloat16 or wider, within the bound.
A program may use at most 32 MiB of HBM per device.

```python
import math
import jax
import jax.numpy as jnp
import numpy as np
from jax import lax

D = 4096
HEADS = 32
HEAD_SIZE = 64
LAYERS = 2
POSITION = 2048
WIDTH = 2048
BATCH = 256


def draw_tokens(key, part):
    key_list = jax.random.split(key, 3)
    row_scale = jnp.exp(jax.random.uniform(key_list[0], (BATCH, 1), jnp.float32, math.log(0.3), math.log(3.0)))
    column_place = jnp.arange(D, dtype=jnp.float32) / D
    jitter = jnp.exp(jax.random.uniform(key_list[1], (1, D), jnp.float32, math.log(0.8), math.log(1.25)))
    column_scale = 0.5 * jnp.exp(column_place * math.log(4.0))[None, :] * jitter
    noise = jnp.clip(jax.random.normal(key_list[2], (BATCH, D), jnp.float32), -4.0, 4.0)
    return (noise * row_scale * column_scale).astype(jnp.bfloat16)


def shard_levels(key, dims, cuts, low, top_value):
    def one(axis_at, blocks):
        draws = jax.random.uniform(jax.random.fold_in(jax.random.fold_in(key, 6), axis_at), (blocks,), jnp.float32, low / len(cuts), top_value / len(cuts))
        return jnp.repeat(jnp.exp(draws), dims[axis_at] // blocks).reshape((-1,) + (1,) * (len(dims) - axis_at - 1))

    factor_of = one(*cuts[0])
    for cut in cuts[1:]:
        factor_of = factor_of * one(*cut)
    return factor_of


def split_up(amount, total, limit, slope):
    portions = [(1 << 20) // math.isqrt(grade ** slope) + 1 for grade in range(2, amount + 1)]
    surplus, holding = total - limit - (amount - 1), [1] * (amount - 1)
    while surplus > 0:
        movable = [i for i in range(amount - 1) if holding[i] < limit]
        whole, remaining = sum([portions[i] for i in movable]), surplus
        for i in movable:
            extra = min(limit - holding[i], max(1, remaining * portions[i] // whole), surplus)
            holding[i] = holding[i] + extra
            surplus = surplus - extra
    return np.array([limit] + holding)


def uneven(rng, amount, total, limit, skew):
    if amount == 2:
        one = jax.random.randint(rng, (), max(1, total - limit), min(limit, total - 1) + 1)
        return jnp.stack([one, total - one])
    sizes = jnp.asarray(split_up(amount, total, limit, skew), jnp.int32)
    twos = (amount - 1) // 2
    giver, receiver = sizes[1:1 + 2 * twos:2], sizes[2:2 + 2 * twos:2]
    room = jnp.minimum(giver - 1, limit - receiver)
    shifted = jax.random.randint(jax.random.fold_in(rng, 1), (twos,), 0, 1 << 20) % (room + 1)
    sizes = sizes.at[1:1 + 2 * twos:2].set(giver - shifted).at[2:2 + 2 * twos:2].set(receiver + shifted)
    return sizes[jax.random.permutation(jax.random.fold_in(rng, 2), amount)]


def centred(key, shape, scale, limit, pieces=(), held_as=jnp.bfloat16):
    result = scale * jax.random.normal(key, shape, jnp.float32)
    if pieces:
        result = result * shard_levels(key, shape, pieces, -0.22, 0.18)
    return jnp.clip(result, -limit, limit).astype(held_as)


def setup_inputs(seed: int = 0) -> dict:
    arg_keys = jax.random.split(jax.random.key(seed), 14)
    return {
        "tokens": draw_tokens(jax.random.fold_in(arg_keys[13], 71), 0),
        "lengths": uneven(arg_keys[1], BATCH, BATCH * POSITION, 4 * POSITION, 2).astype(jnp.int32),
        "in_gain": jnp.clip(1.0 + 0.18 * jax.random.normal(arg_keys[2], (LAYERS, D), jnp.float32), 0.1, 1.9),
        "w_recept": centred(arg_keys[3], (LAYERS, D, WIDTH), D ** -0.5, 0.09375, ((1, 32), (2, 32))),
        "w_key": centred(arg_keys[4], (LAYERS, D, WIDTH), D ** -0.5, 0.09375, ((1, 32), (2, 32))),
        "w_value": centred(arg_keys[5], (LAYERS, D, WIDTH), D ** -0.5, 0.09375, ((1, 32), (2, 32))),
        "w_decay": centred(arg_keys[6], (LAYERS, D, WIDTH), D ** -0.5, 0.09375, ((1, 32), (2, 32))),
        "w_rate": centred(arg_keys[7], (LAYERS, D, WIDTH), D ** -0.5, 0.09375, ((1, 32), (2, 32))),
        "w_gate": centred(arg_keys[8], (LAYERS, D, WIDTH), D ** -0.5, 0.09375, ((1, 32), (2, 32))),
        "w_out": centred(arg_keys[9], (LAYERS, WIDTH, D), WIDTH ** -0.5, 0.125, ((1, 32), (2, 32))),
        "decay_base": centred(arg_keys[10], (LAYERS, WIDTH), 2.0, 6.0, ((1, 32),), jnp.float32),
        "mix_gain": jnp.clip(1.0 + 0.18 * jax.random.normal(arg_keys[11], (LAYERS, WIDTH), jnp.float32), 0.1, 1.9),
        "states": centred(arg_keys[12], (LAYERS, BATCH, HEADS, HEAD_SIZE, HEAD_SIZE), 1.0, 6.0, ((1, 32), (2, 32)), jnp.float32),
    }


DECAY_SCALE = 0.6065306597126334
NORM_EPS = 1e-06
KEY_EPS = 1e-05
GROUP_EPS = 0.00064

def update_heads(projected, previous, base_row, gain_row, alive_rows):
    row_count = previous.shape[0]
    head_count = previous.shape[1]
    head_size = previous.shape[2]
    local_width = head_count * head_size
    role_parts = [projected[:, role_index * local_width:(role_index + 1) * local_width] for role_index in range(6)]
    recept, key_flat, value_flat, decay_pre, rate_pre, gate_pre = role_parts
    decay_factor = jnp.exp(-DECAY_SCALE * jax.nn.sigmoid(decay_pre + base_row))
    in_rate = jax.nn.sigmoid(rate_pre)
    key_heads = key_flat.reshape(row_count, head_count, head_size)
    unit_key = key_heads * lax.rsqrt(lax.optimization_barrier(jnp.sum(key_heads * key_heads, axis=2, keepdims=True)) + KEY_EPS)
    removed = jnp.einsum('bhvk,bhk->bhv', previous, -unit_key, precision=lax.Precision.HIGHEST)
    decay_heads = decay_factor.reshape(row_count, head_count, 1, head_size)
    rate_heads = in_rate.reshape(row_count, head_count, head_size)
    value_heads = value_flat.reshape(row_count, head_count, head_size)
    updated = previous * decay_heads + removed[..., None] * (unit_key * rate_heads)[:, :, None, :] + value_heads[..., None] * key_heads[:, :, None, :]
    recept_heads = recept.reshape(row_count, head_count, head_size)
    readout = jnp.einsum('bhvk,bhk->bhv', updated, recept_heads, precision=lax.Precision.HIGHEST)
    centre = lax.optimization_barrier(jnp.mean(readout, axis=2, keepdims=True))
    spread = lax.optimization_barrier(jnp.mean(jnp.square(readout - centre), axis=2, keepdims=True))
    normed = ((readout - centre) * lax.rsqrt(spread + GROUP_EPS)).reshape(row_count, local_width)
    normed = normed * gain_row * jax.nn.sigmoid(gate_pre)
    mixed_rows = jnp.where(alive_rows[:, None], normed, 0.0).astype(jnp.bfloat16)
    kept_state = jnp.where(alive_rows[:, None, None, None], updated, previous)
    return (mixed_rows, kept_state)

def reference(tokens, lengths, in_gain, w_recept, w_key, w_value, w_decay, w_rate, w_gate, w_out, decay_base, mix_gain, states):
    alive_rows = lengths > POSITION
    current = tokens
    kept_states = []
    for layer_index in range(LAYERS):
        widened = current.astype(jnp.float32)
        inverse = lax.rsqrt(lax.optimization_barrier(jnp.mean(widened * widened, axis=1, keepdims=True)) + NORM_EPS)
        scaled = (widened * in_gain[layer_index]).astype(jnp.bfloat16)
        outputs = [jnp.dot(scaled, weight[layer_index], preferred_element_type=jnp.float32) * inverse for weight in (w_recept, w_key, w_value, w_decay, w_rate, w_gate)]
        projected = jnp.concatenate(outputs, axis=1)
        mixed_rows, kept_state = update_heads(projected, states[layer_index], decay_base[layer_index], mix_gain[layer_index], alive_rows)
        branch = jnp.dot(mixed_rows, w_out[layer_index], preferred_element_type=jnp.float32)
        current = (widened + branch).astype(jnp.bfloat16)
        kept_states.append(kept_state)
    return (current, jnp.stack(kept_states))
```

```python
import jax
import jax.numpy as jnp
from jax import lax
from jax.experimental import pallas as pl
from jax.experimental.pallas import tpu as pltpu
from jax.sharding import PartitionSpec as P

D = 4096
LAYERS = 2
POSITION = 2048
HEAD = 64
ROWS = 8

DECAY_SCALE = 0.6065306597126334
NORM_EPS = 1e-06
KEY_EPS = 1e-05
GROUP_EPS = 0.00064

TP = 32
YS = 8
XS = 4

BF16 = jnp.bfloat16
F32 = jnp.float32


def sigmoid(v):
    return 1.0 / (1.0 + jnp.exp(-v))


def kernel(
    tok_hbm,
    len_smem,
    gain_hbm,
    wr_hbm,
    wk_hbm,
    wv_hbm,
    wd_hbm,
    wa_hbm,
    wg_hbm,
    wo_hbm,
    base_hbm,
    mix_hbm,
    state_hbm,
    next_out,
    state_out,
    tok,
    gain,
    wstage,
    wall,
    wout,
    base,
    mixg,
    prev,
    kept,
    x0,
    x1,
    pb_send,
    pb_recv,
    mb_send,
    mb_recv,
    ob_send,
    sum_recv,
    fin_recv,
    own_new,
    resid,
    load_sem,
    state_sem,
    out_sem,
    send_sem,
    gather_sem,
    x_sem,
    p_sem,
    m_sem,
    d_sem,
    r_sem,
):
    t = lax.axis_index("tp")
    dp = lax.axis_index("dp")
    y = dp // XS
    x = lax.rem(dp, XS)
    home = lax.rem(t, XS)
    group = t // XS
    is_owner = home == x

    def dev(tt, yy, xx):
        return {"tp": tt, "dp": yy * XS + xx}

    def wrap(v, n):
        return lax.rem(v + n, n)

    small = [
        (tok_hbm, tok),
        (gain_hbm, gain.at[x]),
        (wr_hbm, wstage.at[0]),
        (wk_hbm, wstage.at[1]),
        (wv_hbm, wstage.at[2]),
        (wd_hbm, wstage.at[3]),
        (wa_hbm, wstage.at[4]),
        (wg_hbm, wstage.at[5]),
        (wo_hbm, wout.at[x]),
        (base_hbm, base),
        (mix_hbm, mixg),
    ]
    loads = [
        pltpu.make_async_copy(src, dst, load_sem.at[i])
        for i, (src, dst) in enumerate(small)
    ]
    for load in loads:
        load.start()
    state_load = pltpu.make_async_copy(state_hbm, prev, state_sem)
    state_load.start()

    barrier = pltpu.get_barrier_semaphore()

    def greet(i, _):
        tt = wrap(t + i, TP)

        @pl.when(jnp.logical_or(i != 0, jnp.logical_not(is_owner)))
        def _():
            pl.semaphore_signal(barrier, 1, device_id=dev(tt, y, home))

        a = lax.rem(group + i // XS, YS)
        xx = wrap(x + lax.rem(i, XS), XS)

        @pl.when(jnp.logical_or(i != 0, jnp.logical_not(is_owner)))
        def _():
            pl.semaphore_signal(barrier, 1, device_id=dev(a * XS + x, y, xx))

        return 0

    lax.fori_loop(0, TP, greet, 0)
    for i in range(1, XS):
        pl.semaphore_signal(barrier, 1, device_id=dev(t, y, wrap(x + i, XS)))
    for i in range(1, YS):
        pl.semaphore_signal(barrier, 1, device_id=dev(t, wrap(y + i, YS), x))

    for load in loads:
        load.wait()
    for layer in range(LAYERS):
        for pair in range(3):
            wall[layer, x, :, pair * 128 : pair * 128 + 128] = jnp.concatenate(
                [wstage[2 * pair, layer], wstage[2 * pair + 1, layer]], axis=1
            )

    own = jnp.where(is_owner, 1, 0)
    pl.semaphore_wait(barrier, 2 * (TP - own) + (XS - 1) + (YS - 1))

    slot = x * YS + group

    def send_tokens(i, _):
        tt = wrap(t + TP // 2 + i, TP)
        pltpu.make_async_remote_copy(
            tok, x0.at[slot], send_sem.at[0], x_sem.at[0], device_id=dev(tt, y, home)
        ).start()
        return 0

    def send_tokens_skip(i, _):
        @pl.when(i != TP // 2)
        def _():
            send_tokens(i, 0)

        return 0

    lax.fori_loop(0, TP, send_tokens_skip, 0)

    @pl.when(is_owner)
    def _():
        pltpu.make_async_copy(tok, x0.at[slot], x_sem.at[0]).start()

    @pl.when(jnp.logical_not(is_owner))
    def _():
        send_tokens(TP // 2, 0)

    for layer in range(LAYERS):
        for i in (2, 1, 3):
            to = dev(t, y, wrap(x + i, XS))
            pltpu.make_async_remote_copy(
                wall.at[layer, x], wall.at[layer, x], send_sem.at[1], gather_sem.at[layer], device_id=to
            ).start()
        if layer == 0:
            for i in (2, 1, 3):
                to = dev(t, y, wrap(x + i, XS))
                pltpu.make_async_remote_copy(
                    gain.at[x], gain.at[x], send_sem.at[2], gather_sem.at[2], device_id=to
                ).start()
                pltpu.make_async_remote_copy(
                    wout.at[x], wout.at[x], send_sem.at[3], gather_sem.at[3], device_id=to
                ).start()

    def arrived(ref, sem):
        pltpu.make_async_copy(ref, ref, sem).wait()

    rows = lax.broadcasted_iota(jnp.int32, (ROWS, HEAD), 0)
    held = jnp.zeros((ROWS, HEAD), jnp.int32)
    for b in range(ROWS):
        held = jnp.where(rows == b, len_smem[b], held)
    live_rows = held > POSITION
    eye = (
        lax.broadcasted_iota(jnp.int32, (HEAD, HEAD), 0)
        == lax.broadcasted_iota(jnp.int32, (HEAD, HEAD), 1)
    ).astype(F32)

    state_load.wait()

    for layer in range(LAYERS):
        if layer == 0:
            arrived(gain.at[0:3], gather_sem.at[2])
            arrived(x0, x_sem.at[0])
            blocks = [
                x0[f * YS : (f + 1) * YS].astype(F32).reshape(YS * ROWS, 128)
                for f in range(XS)
            ]
        else:
            arrived(x1, x_sem.at[1])
            blocks = [x1[:, f].astype(F32).reshape(YS * ROWS, 128) for f in range(XS)]
        total = blocks[0] * blocks[0]
        for f in range(1, XS):
            total = total + blocks[f] * blocks[f]
        squares = jnp.sum(total, axis=1, keepdims=True)
        scaled = jnp.concatenate(
            [
                (blocks[f] * gain[f, layer : layer + 1, :]).astype(BF16)
                for f in range(XS)
            ],
            axis=1,
        )
        arrived(wall.at[layer, 0:3], gather_sem.at[layer])
        weights = wall[layer].reshape(XS * 128, 6 * HEAD)
        partial = jnp.dot(scaled, weights, preferred_element_type=F32)
        coarse = squares.astype(BF16).astype(F32)
        fine = squares - coarse
        lanes = lax.broadcasted_iota(jnp.int32, (YS * ROWS, 128), 1)
        tail = jnp.where(lanes < HEAD, coarse, fine)
        pb_send[layer, :, :, 0 : 6 * HEAD] = partial.reshape(YS, ROWS, 6 * HEAD).astype(BF16)
        pb_send[layer, :, :, 6 * HEAD :] = tail.reshape(YS, ROWS, 128).astype(BF16)
        for i in (4, 3, 5, 2, 6, 1, 7):
            yy = wrap(y + i, YS)
            pltpu.make_async_remote_copy(
                pb_send.at[layer, yy],
                pb_recv.at[layer, y],
                send_sem.at[4 + layer],
                p_sem.at[layer],
                device_id=dev(t, yy, x),
            ).start()
        pb_recv[layer, y] = pb_send[layer, y]
        arrived(pb_recv.at[layer, 0:7], p_sem.at[layer])
        summed = pb_recv[layer, 0].astype(F32)
        for i in range(1, YS):
            summed = summed + pb_recv[layer, i].astype(F32)
        sq = summed[:, 6 * HEAD : 6 * HEAD + 1] + summed[:, 7 * HEAD : 7 * HEAD + 1]
        projected = summed * lax.rsqrt(sq / D + NORM_EPS)
        recept, key, value, decay_pre, rate_pre, gate_pre = [
            projected[:, j * HEAD : (j + 1) * HEAD] for j in range(6)
        ]
        decay = jnp.exp(-DECAY_SCALE * sigmoid(decay_pre + base[layer : layer + 1, :]))
        unit = key * lax.rsqrt(jnp.sum(key * key, axis=1, keepdims=True) + KEY_EPS)
        correction = unit * sigmoid(rate_pre)
        readouts = []
        for b in range(ROWS):
            one = slice(b, b + 1)
            state = prev[layer, b]
            removed = -jnp.sum(state * unit[one], axis=1, keepdims=True)
            value_col = jnp.sum(eye * value[one], axis=1, keepdims=True)
            updated = state * decay[one] + removed * correction[one] + value_col * key[one]
            read = jnp.sum(updated * recept[one], axis=1, keepdims=True)
            readouts.append(jnp.sum(eye * read, axis=0, keepdims=True))
            alive = jnp.full((HEAD, HEAD), len_smem[b], jnp.int32) > POSITION
            kept[layer, b] = jnp.where(alive, updated, state)
        pltpu.make_async_copy(kept.at[layer], state_out.at[layer], out_sem.at[layer]).start()
        readout = jnp.concatenate(readouts, axis=0)
        centre = jnp.sum(readout, axis=1, keepdims=True) / HEAD
        off = readout - centre
        spread = jnp.sum(off * off, axis=1, keepdims=True) / HEAD
        normed = off * lax.rsqrt(spread + GROUP_EPS)
        normed = normed * mixg[layer : layer + 1, :] * sigmoid(gate_pre)
        mixed = jnp.where(live_rows, normed, 0.0)
        mb_send[layer] = jnp.concatenate([mixed, mixed], axis=1).astype(BF16)
        for i in (4, 3, 5, 2, 6, 1, 7):
            yy = wrap(y + i, YS)
            pltpu.make_async_remote_copy(
                mb_send.at[layer],
                mb_recv.at[layer, y],
                send_sem.at[6 + layer],
                m_sem.at[layer],
                device_id=dev(t, yy, x),
            ).start()
        mb_recv[layer, y] = mb_send[layer]
        if layer == 0:
            arrived(wout.at[0:3], gather_sem.at[3])
        arrived(mb_recv.at[layer, 0:7], m_sem.at[layer])
        everyone = mb_recv[layer].astype(F32).reshape(YS * ROWS, 128)[:, :HEAD].astype(BF16)
        for f in range(XS):
            term = jnp.dot(everyone, wout[f, layer], preferred_element_type=F32)
            ob_send[layer, :, f] = term.reshape(YS, ROWS, 128).astype(BF16)

        if layer == 0:
            def send_sums(i, _):
                a = wrap(group + YS // 2 + i, YS)

                @pl.when(jnp.logical_or(i != YS // 2, jnp.logical_not(is_owner)))
                def _():
                    pltpu.make_async_remote_copy(
                        ob_send.at[0, a],
                        sum_recv.at[t],
                        send_sem.at[8],
                        d_sem.at[0],
                        device_id=dev(a * XS + x, y, x),
                    ).start()

                return 0

            lax.fori_loop(0, YS, send_sums, 0)

            @pl.when(is_owner)
            def _():
                sum_recv[t] = ob_send[0, group]
                arrived(sum_recv.at[0 : TP - 1], d_sem.at[0])
                acc = sum_recv[0].astype(F32)
                for i in range(1, TP):
                    acc = acc + sum_recv[i].astype(F32)
                for f in range(XS):
                    own_new[f] = (x0[f * YS + group].astype(F32) + acc[f]).astype(BF16)

                def send_new(i, _):
                    tt = wrap(t + TP // 2 + i, TP)

                    @pl.when(i != TP // 2)
                    def _():
                        pltpu.make_async_remote_copy(
                            own_new,
                            x1.at[group],
                            send_sem.at[9],
                            x_sem.at[1],
                            device_id=dev(tt, y, x),
                        ).start()

                    return 0

                lax.fori_loop(0, TP, send_new, 0)
                pltpu.make_async_copy(own_new, x1.at[group], x_sem.at[1]).start()
                for i in range(1, XS):
                    xx = wrap(x + i, XS)
                    pltpu.make_async_remote_copy(
                        own_new.at[xx],
                        resid,
                        send_sem.at[10],
                        r_sem,
                        device_id=dev(t, y, xx),
                    ).start()
                pltpu.make_async_copy(own_new.at[x], resid, r_sem).start()

        else:
            def send_last(i, _):
                a = wrap(group + YS // 2 + i // XS, YS)
                xx = wrap(x + lax.rem(i, XS), XS)

                @pl.when(jnp.logical_or(i != TP // 2, jnp.logical_not(is_owner)))
                def _():
                    pltpu.make_async_remote_copy(
                        ob_send.at[1, a, xx],
                        fin_recv.at[t],
                        send_sem.at[11],
                        d_sem.at[1],
                        device_id=dev(a * XS + x, y, xx),
                    ).start()

                return 0

            lax.fori_loop(0, TP, send_last, 0)

            @pl.when(is_owner)
            def _():
                pltpu.make_async_copy(
                    ob_send.at[1, group, x], fin_recv.at[t], d_sem.at[1]
                ).start()

            arrived(resid, r_sem)
            arrived(fin_recv, d_sem.at[1])
            acc = fin_recv[0].astype(F32)
            for i in range(1, TP):
                acc = acc + fin_recv[i].astype(F32)
            next_out[...] = (resid[...].astype(F32) + acc).astype(BF16)

    arrived(x0.at[0 : TP - 1], send_sem.at[0])

    @pl.when(jnp.logical_not(is_owner))
    def _():
        arrived(x0.at[0], send_sem.at[0])
        arrived(ob_send.at[0, 0], send_sem.at[8])
        arrived(fin_recv.at[0], send_sem.at[11])

    @pl.when(is_owner)
    def _():
        arrived(sum_recv.at[0 : TP - 1], send_sem.at[9])
        arrived(own_new.at[0:3], send_sem.at[10])

    for layer in range(LAYERS):
        arrived(wall.at[layer, 0:3], send_sem.at[1])
        arrived(pb_recv.at[layer, 0:7], send_sem.at[4 + layer])
        arrived(mb_recv.at[layer, 0:7], send_sem.at[6 + layer])
        pltpu.make_async_copy(kept.at[layer], state_out.at[layer], out_sem.at[layer]).wait()
    arrived(gain.at[0:3], send_sem.at[2])
    arrived(wout.at[0:3], send_sem.at[3])
    arrived(ob_send.at[0, 0:7], send_sem.at[8])
    arrived(fin_recv.at[0 : TP - 1], send_sem.at[11])


def on_device(
    tokens,
    lengths,
    in_gain,
    w_recept,
    w_key,
    w_value,
    w_decay,
    w_rate,
    w_gate,
    w_out,
    decay_base,
    mix_gain,
    states,
):
    hbm = pl.BlockSpec(memory_space=pl.ANY)
    vmem = pltpu.VMEM
    dma = pltpu.SemaphoreType.DMA
    squeezed = states.reshape(LAYERS, ROWS, HEAD, HEAD)
    next_tokens, new_states = pl.pallas_call(
        kernel,
        out_shape=(
            jax.ShapeDtypeStruct(tokens.shape, BF16),
            jax.ShapeDtypeStruct(squeezed.shape, F32),
        ),
        in_specs=[hbm, pl.BlockSpec(memory_space=pltpu.SMEM)] + [hbm] * 11,
        out_specs=(pl.BlockSpec(memory_space=pltpu.VMEM), hbm),
        scratch_shapes=[
            vmem((ROWS, 128), BF16),
            vmem((XS, LAYERS, 128), F32),
            vmem((6, LAYERS, 128, HEAD), BF16),
            vmem((LAYERS, XS, 128, 6 * HEAD), BF16),
            vmem((XS, LAYERS, HEAD, 128), BF16),
            vmem((LAYERS, HEAD), F32),
            vmem((LAYERS, HEAD), F32),
            vmem((LAYERS, ROWS, HEAD, HEAD), F32),
            vmem((LAYERS, ROWS, HEAD, HEAD), F32),
            vmem((XS * YS, ROWS, 128), BF16),
            vmem((YS, XS, ROWS, 128), BF16),
            vmem((LAYERS, YS, ROWS, 512), BF16),
            vmem((LAYERS, YS, ROWS, 512), BF16),
            vmem((LAYERS, ROWS, 128), BF16),
            vmem((LAYERS, YS, ROWS, 128), BF16),
            vmem((LAYERS, YS, XS, ROWS, 128), BF16),
            vmem((TP, XS, ROWS, 128), BF16),
            vmem((TP, ROWS, 128), BF16),
            vmem((XS, ROWS, 128), BF16),
            vmem((ROWS, 128), BF16),
            dma((11,)),
            dma(()),
            dma((LAYERS,)),
            dma((12,)),
            dma((4,)),
            dma((2,)),
            dma((LAYERS,)),
            dma((LAYERS,)),
            dma((2,)),
            dma(()),
        ],
        compiler_params=pltpu.CompilerParams(collective_id=0, has_side_effects=True),
        name="decode_step",
    )(
        tokens,
        lengths,
        in_gain,
        w_recept,
        w_key,
        w_value,
        w_decay,
        w_rate,
        w_gate,
        w_out,
        decay_base,
        mix_gain,
        squeezed,
    )
    return (next_tokens, new_states.reshape(states.shape))


def solution(mesh):
    in_specs = (
        P("tp", "dp"),
        P("dp"),
        P(None, "dp"),
        P(None, "dp", "tp"),
        P(None, "dp", "tp"),
        P(None, "dp", "tp"),
        P(None, "dp", "tp"),
        P(None, "dp", "tp"),
        P(None, "dp", "tp"),
        P(None, "tp", "dp"),
        P(None, "tp"),
        P(None, "tp"),
        P(None, "dp", "tp", None, None),
    )
    out_specs = (P("tp", "dp"), P(None, "dp", "tp", None, None))
    return jax.shard_map(
        on_device, mesh=mesh, in_specs=in_specs, out_specs=out_specs, check_vma=False
    )
```

```python
import jax
import jax.numpy as jnp
from jax import lax
from jax.experimental import pallas as pl
from jax.experimental.pallas import tpu as pltpu
from jax.sharding import PartitionSpec as P

D = 4096
LAYERS = 2
POSITION = 2048
HEAD = 64
ROWS = 8

DECAY_SCALE = 0.6065306597126334
NORM_EPS = 1e-06
KEY_EPS = 1e-05
GROUP_EPS = 0.00064

TP = 32
YS = 8
XS = 4

BF16 = jnp.bfloat16
F32 = jnp.float32


def sigmoid(v):
    return 1.0 / (1.0 + jnp.exp(-v))


def kernel(
    tok_hbm,
    len_smem,
    gain_hbm,
    wr_hbm,
    wk_hbm,
    wv_hbm,
    wd_hbm,
    wa_hbm,
    wg_hbm,
    wo_hbm,
    base_hbm,
    mix_hbm,
    state_hbm,
    next_out,
    state_out,
    tok,
    gain,
    wall,
    wout,
    base,
    mixg,
    prev,
    x0,
    x1,
    pb_send,
    pb_recv,
    mb_send,
    mb_recv,
    ob_send,
    sum_recv,
    fin_recv,
    own_new,
    resid,
    load_sem,
    state_sem,
    send_sem,
    gather_sem,
    x_sem,
    p_sem,
    m_sem,
    d_sem,
    r_sem,
):
    t = lax.axis_index("tp")
    dp = lax.axis_index("dp")
    y = dp // XS
    x = lax.rem(dp, XS)
    home = lax.rem(t, XS)
    group = t // XS
    is_owner = home == x

    def dev(tt, yy, xx):
        return {"tp": tt, "dp": yy * XS + xx}

    def wrap(v, n):
        return lax.rem(v + n, n)

    token_load = pltpu.make_async_copy(tok_hbm, tok, load_sem.at[0])
    token_load.start()
    loads = []
    for layer in range(LAYERS):
        for j, ref in enumerate((wr_hbm, wk_hbm, wv_hbm, wd_hbm, wa_hbm, wg_hbm)):
            loads.append((ref.at[layer], wall.at[layer, x, j * HEAD : (j + 1) * HEAD]))
    loads += [
        (gain_hbm, gain.at[x]),
        (wo_hbm, wout.at[x]),
        (base_hbm, base),
        (mix_hbm, mixg),
    ]
    loads = [
        pltpu.make_async_copy(src, dst, load_sem.at[1 + i])
        for i, (src, dst) in enumerate(loads)
    ]
    for load in loads:
        load.start()
    state_load = pltpu.make_async_copy(state_hbm, prev, state_sem)
    state_load.start()

    barrier = pltpu.get_barrier_semaphore()

    def ring(i):
        step = (i + 1) // 2
        return TP // 2 + jnp.where(lax.rem(i, 2) == 1, step, -step)

    def greet(i, _):
        tt = wrap(t + ring(i), TP)
        pl.semaphore_signal(barrier, 1, device_id=dev(tt, y, home))
        return 0

    lax.fori_loop(0, TP - 1, greet, 0)

    def greet_back(i, _):
        a = wrap(group + YS // 2 + i // XS, YS)
        xx = wrap(x + lax.rem(i, XS), XS)

        @pl.when(jnp.logical_or(i != TP // 2, jnp.logical_not(is_owner)))
        def _():
            pl.semaphore_signal(barrier, 1, device_id=dev(a * XS + x, y, xx))

        return 0

    lax.fori_loop(0, TP, greet_back, 0)

    @pl.when(jnp.logical_not(is_owner))
    def _():
        pl.semaphore_signal(barrier, 1, device_id=dev(t, y, home))

    for i in range(1, XS):
        pl.semaphore_signal(barrier, 1, device_id=dev(t, y, wrap(x + i, XS)))
    for i in range(1, YS):
        pl.semaphore_signal(barrier, 1, device_id=dev(t, wrap(y + i, YS), x))

    token_load.wait()

    own = jnp.where(is_owner, 1, 0)
    pl.semaphore_wait(barrier, 2 * (TP - own) + (XS - 1) + (YS - 1))

    slot = x * YS + group

    def send_tokens(i, _):
        tt = wrap(t + ring(i), TP)
        pltpu.make_async_remote_copy(
            tok, x0.at[slot], send_sem.at[0], x_sem.at[0], device_id=dev(tt, y, home)
        ).start()
        return 0

    lax.fori_loop(0, TP - 1, send_tokens, 0)

    @pl.when(is_owner)
    def _():
        pltpu.make_async_copy(tok, x0.at[slot], x_sem.at[0]).start()

    @pl.when(jnp.logical_not(is_owner))
    def _():
        send_tokens(TP - 1, 0)

    for load in loads:
        load.wait()

    for layer in range(LAYERS):
        for i in (2, 1, 3):
            to = dev(t, y, wrap(x + i, XS))
            pltpu.make_async_remote_copy(
                wall.at[layer, x], wall.at[layer, x], send_sem.at[1], gather_sem.at[layer], device_id=to
            ).start()
        if layer == 0:
            for i in (2, 1, 3):
                to = dev(t, y, wrap(x + i, XS))
                pltpu.make_async_remote_copy(
                    gain.at[x], gain.at[x], send_sem.at[2], gather_sem.at[2], device_id=to
                ).start()
                pltpu.make_async_remote_copy(
                    wout.at[x], wout.at[x], send_sem.at[3], gather_sem.at[3], device_id=to
                ).start()

    def arrived(ref, sem):
        pltpu.make_async_copy(ref, ref, sem).wait()

    rows = lax.broadcasted_iota(jnp.int32, (ROWS, HEAD), 0)
    held = jnp.zeros((ROWS, HEAD), jnp.int32)
    for b in range(ROWS):
        held = jnp.where(rows == b, len_smem[b], held)
    live_rows = held > POSITION
    eye = (
        lax.broadcasted_iota(jnp.int32, (HEAD, HEAD), 0)
        == lax.broadcasted_iota(jnp.int32, (HEAD, HEAD), 1)
    ).astype(F32)

    state_load.wait()

    for layer in range(LAYERS):
        if layer == 0:
            arrived(gain.at[0:3], gather_sem.at[2])
            arrived(x0, x_sem.at[0])
            blocks = [
                x0[f * YS : (f + 1) * YS].astype(F32).reshape(YS * ROWS, 128)
                for f in range(XS)
            ]
        else:
            arrived(x1, x_sem.at[1])
            blocks = [x1[:, f].astype(F32).reshape(YS * ROWS, 128) for f in range(XS)]
        total = blocks[0] * blocks[0]
        for f in range(1, XS):
            total = total + blocks[f] * blocks[f]
        squares = jnp.sum(total, axis=1, keepdims=True)
        arrived(wall.at[layer, 0:3], gather_sem.at[layer])
        partial = None
        for f in range(XS):
            term = lax.dot_general(
                (blocks[f] * gain[f, layer : layer + 1, :]).astype(BF16),
                wall[layer, f],
                (((1,), (1,)), ((), ())),
                preferred_element_type=F32,
            )
            partial = term if partial is None else partial + term
        coarse = squares.astype(BF16).astype(F32)
        fine = squares - coarse
        lanes = lax.broadcasted_iota(jnp.int32, (YS * ROWS, 128), 1)
        tail = jnp.where(lanes < HEAD, coarse, fine)
        pb_send[layer, :, :, 0 : 6 * HEAD] = partial.reshape(YS, ROWS, 6 * HEAD).astype(BF16)
        pb_send[layer, :, :, 6 * HEAD :] = tail.reshape(YS, ROWS, 128).astype(BF16)
        for i in (4, 3, 5, 2, 6, 1, 7):
            yy = wrap(y + i, YS)
            pltpu.make_async_remote_copy(
                pb_send.at[layer, yy],
                pb_recv.at[layer, y],
                send_sem.at[4 + layer],
                p_sem.at[layer],
                device_id=dev(t, yy, x),
            ).start()
        pb_recv[layer, y] = pb_send[layer, y]
        arrived(pb_recv.at[layer, 0:7], p_sem.at[layer])
        summed = pb_recv[layer, 0].astype(F32)
        for i in range(1, YS):
            summed = summed + pb_recv[layer, i].astype(F32)
        sq = summed[:, 6 * HEAD : 6 * HEAD + 1] + summed[:, 7 * HEAD : 7 * HEAD + 1]
        projected = summed * lax.rsqrt(sq / D + NORM_EPS)
        recept, key, value, decay_pre, rate_pre, gate_pre = [
            projected[:, j * HEAD : (j + 1) * HEAD] for j in range(6)
        ]
        decay = jnp.exp(-DECAY_SCALE * sigmoid(decay_pre + base[layer : layer + 1, :]))
        unit = key * lax.rsqrt(jnp.sum(key * key, axis=1, keepdims=True) + KEY_EPS)
        correction = unit * sigmoid(rate_pre)
        read_key = decay * recept
        read_fix = jnp.sum(correction * recept, axis=1, keepdims=True)
        read_value = jnp.sum(key * recept, axis=1, keepdims=True)
        removals = []
        reads = []
        for b in range(ROWS):
            one = slice(b, b + 1)
            state = prev[layer, b]
            removed = -jnp.sum(state * unit[one], axis=1, keepdims=True)
            read = jnp.sum(state * read_key[one], axis=1, keepdims=True)
            removals.append(removed)
            read = read + removed * read_fix[one]
            reads.append(jnp.sum(eye * read, axis=0, keepdims=True))
        readout = jnp.concatenate(reads, axis=0) + value * read_value
        centre = jnp.sum(readout, axis=1, keepdims=True) / HEAD
        off = readout - centre
        spread = jnp.sum(off * off, axis=1, keepdims=True) / HEAD
        normed = off * lax.rsqrt(spread + GROUP_EPS)
        normed = normed * mixg[layer : layer + 1, :] * sigmoid(gate_pre)
        mixed = jnp.where(live_rows, normed, 0.0)
        mb_send[layer] = jnp.concatenate([mixed, mixed], axis=1).astype(BF16)
        for i in (4, 3, 5, 2, 6, 1, 7):
            yy = wrap(y + i, YS)
            pltpu.make_async_remote_copy(
                mb_send.at[layer],
                mb_recv.at[layer, y],
                send_sem.at[6 + layer],
                m_sem.at[layer],
                device_id=dev(t, yy, x),
            ).start()
        mb_recv[layer, y] = mb_send[layer]
        for b in range(ROWS):
            one = slice(b, b + 1)
            state = prev[layer, b]
            value_col = jnp.sum(eye * value[one], axis=1, keepdims=True)
            updated = (
                state * decay[one] + removals[b] * correction[one] + value_col * key[one]
            )
            alive = jnp.full((HEAD, HEAD), len_smem[b], jnp.int32) > POSITION
            state_out[layer, b] = jnp.where(alive, updated, state)
        if layer == 0:
            arrived(wout.at[0:3], gather_sem.at[3])
        arrived(mb_recv.at[layer, 0:7], m_sem.at[layer])
        everyone = mb_recv[layer].astype(F32).reshape(YS * ROWS, 128)[:, :HEAD].astype(BF16)
        for f in range(XS):
            term = jnp.dot(everyone, wout[f, layer], preferred_element_type=F32)
            ob_send[layer, :, f] = term.reshape(YS, ROWS, 128).astype(BF16)

        if layer == 0:
            def send_sums(i, _):
                a = wrap(group + YS // 2 + i, YS)

                @pl.when(jnp.logical_or(i != YS // 2, jnp.logical_not(is_owner)))
                def _():
                    pltpu.make_async_remote_copy(
                        ob_send.at[0, a],
                        sum_recv.at[t],
                        send_sem.at[8],
                        d_sem.at[0],
                        device_id=dev(a * XS + x, y, x),
                    ).start()

                return 0

            lax.fori_loop(0, YS, send_sums, 0)

            @pl.when(is_owner)
            def _():
                sum_recv[t] = ob_send[0, group]
                arrived(sum_recv.at[0 : TP - 1], d_sem.at[0])
                acc = sum_recv[0].astype(F32)
                for i in range(1, TP):
                    acc = acc + sum_recv[i].astype(F32)
                for f in range(XS):
                    own_new[f] = (x0[f * YS + group].astype(F32) + acc[f]).astype(BF16)

                def send_new(i, _):
                    tt = wrap(t + TP // 2 + i, TP)

                    @pl.when(i != TP // 2)
                    def _():
                        pltpu.make_async_remote_copy(
                            own_new,
                            x1.at[group],
                            send_sem.at[9],
                            x_sem.at[1],
                            device_id=dev(tt, y, x),
                        ).start()

                    return 0

                lax.fori_loop(0, TP, send_new, 0)
                pltpu.make_async_copy(own_new, x1.at[group], x_sem.at[1]).start()
                for i in range(1, XS):
                    xx = wrap(x + i, XS)
                    pltpu.make_async_remote_copy(
                        own_new.at[xx],
                        resid,
                        send_sem.at[10],
                        r_sem,
                        device_id=dev(t, y, xx),
                    ).start()
                pltpu.make_async_copy(own_new.at[x], resid, r_sem).start()

        else:
            def send_last(i, _):
                a = wrap(group + YS // 2 + i // XS, YS)
                xx = wrap(x + lax.rem(i, XS), XS)

                @pl.when(jnp.logical_or(i != TP // 2, jnp.logical_not(is_owner)))
                def _():
                    pltpu.make_async_remote_copy(
                        ob_send.at[1, a, xx],
                        fin_recv.at[t],
                        send_sem.at[11],
                        d_sem.at[1],
                        device_id=dev(a * XS + x, y, xx),
                    ).start()

                return 0

            lax.fori_loop(0, TP, send_last, 0)

            @pl.when(is_owner)
            def _():
                pltpu.make_async_copy(
                    ob_send.at[1, group, x], fin_recv.at[t], d_sem.at[1]
                ).start()

            arrived(resid, r_sem)
            arrived(fin_recv, d_sem.at[1])
            acc = fin_recv[0].astype(F32)
            for i in range(1, TP):
                acc = acc + fin_recv[i].astype(F32)
            next_out[...] = (resid[...].astype(F32) + acc).astype(BF16)

    arrived(x0.at[0 : TP - 1], send_sem.at[0])

    @pl.when(jnp.logical_not(is_owner))
    def _():
        arrived(x0.at[0], send_sem.at[0])
        arrived(ob_send.at[0, 0], send_sem.at[8])
        arrived(fin_recv.at[0], send_sem.at[11])

    @pl.when(is_owner)
    def _():
        arrived(sum_recv.at[0 : TP - 1], send_sem.at[9])
        arrived(own_new.at[0:3], send_sem.at[10])

    for layer in range(LAYERS):
        arrived(wall.at[layer, 0:3], send_sem.at[1])
        arrived(pb_recv.at[layer, 0:7], send_sem.at[4 + layer])
        arrived(mb_recv.at[layer, 0:7], send_sem.at[6 + layer])
    arrived(gain.at[0:3], send_sem.at[2])
    arrived(wout.at[0:3], send_sem.at[3])
    arrived(ob_send.at[0, 0:7], send_sem.at[8])
    arrived(fin_recv.at[0 : TP - 1], send_sem.at[11])


def on_device(
    tokens,
    lengths,
    in_gain,
    w_recept,
    w_key,
    w_value,
    w_decay,
    w_rate,
    w_gate,
    w_out,
    decay_base,
    mix_gain,
    states,
):
    hbm = pl.BlockSpec(memory_space=pl.ANY)
    vmem = pltpu.VMEM
    dma = pltpu.SemaphoreType.DMA
    turned = [
        jnp.swapaxes(w, 1, 2)
        for w in (w_recept, w_key, w_value, w_decay, w_rate, w_gate)
    ]
    squeezed = states.reshape(LAYERS, ROWS, HEAD, HEAD)
    next_tokens, new_states = pl.pallas_call(
        kernel,
        out_shape=(
            pltpu.VMEM(tokens.shape, BF16),
            pltpu.VMEM(squeezed.shape, F32),
        ),
        in_specs=[hbm, pl.BlockSpec(memory_space=pltpu.SMEM)] + [hbm] * 11,
        out_specs=(pl.BlockSpec(memory_space=pltpu.VMEM), pl.BlockSpec(memory_space=pltpu.VMEM)),
        scratch_shapes=[
            vmem((ROWS, 128), BF16),
            vmem((XS, LAYERS, 128), F32),
            vmem((LAYERS, XS, 6 * HEAD, 128), BF16),
            vmem((XS, LAYERS, HEAD, 128), BF16),
            vmem((LAYERS, HEAD), F32),
            vmem((LAYERS, HEAD), F32),
            vmem((LAYERS, ROWS, HEAD, HEAD), F32),
            vmem((XS * YS, ROWS, 128), BF16),
            vmem((YS, XS, ROWS, 128), BF16),
            vmem((LAYERS, YS, ROWS, 512), BF16),
            vmem((LAYERS, YS, ROWS, 512), BF16),
            vmem((LAYERS, ROWS, 128), BF16),
            vmem((LAYERS, YS, ROWS, 128), BF16),
            vmem((LAYERS, YS, XS, ROWS, 128), BF16),
            vmem((TP, XS, ROWS, 128), BF16),
            vmem((TP, ROWS, 128), BF16),
            vmem((XS, ROWS, 128), BF16),
            vmem((ROWS, 128), BF16),
            dma((17,)),
            dma(()),
            dma((12,)),
            dma((4,)),
            dma((2,)),
            dma((LAYERS,)),
            dma((LAYERS,)),
            dma((2,)),
            dma(()),
        ],
        compiler_params=pltpu.CompilerParams(collective_id=0, has_side_effects=True),
        name="decode_step",
    )(
        tokens,
        lengths,
        in_gain,
        *turned,
        w_out,
        decay_base,
        mix_gain,
        squeezed,
    )
    return (next_tokens, new_states.reshape(states.shape))


def solution(mesh):
    in_specs = (
        P("tp", "dp"),
        P("dp"),
        P(None, "dp"),
        P(None, "dp", "tp"),
        P(None, "dp", "tp"),
        P(None, "dp", "tp"),
        P(None, "dp", "tp"),
        P(None, "dp", "tp"),
        P(None, "dp", "tp"),
        P(None, "tp", "dp"),
        P(None, "tp"),
        P(None, "tp"),
        P(None, "dp", "tp", None, None),
    )
    out_specs = (P("tp", "dp"), P(None, "dp", "tp", None, None))
    return jax.shard_map(
        on_device, mesh=mesh, in_specs=in_specs, out_specs=out_specs, check_vma=False
    )
```
